512 devices in a mesh: sp: 16 (over z), dp: 32 (over y, x, core).
Axes of the slice: x: 4, y: 4, z: 16, core: 2. Of those that a mesh axis runs over, the one named last changes fastest.
Arguments:
- normed: bfloat16 [32, 2048, 2048], P('dp', 'sp'), may hold values from -6 to 6
- values: bfloat16 [32, 2048, 2048], P('dp', 'sp'), may hold values from -6 to 6
- gate_in: bfloat16 [32, 2048, 2048], P('dp', 'sp'), may hold values from -6 to 6
- step_raw: bfloat16 [32, 2048, 32], P('dp', 'sp'), may hold values from -3.5 to 2.5
- upstream: bfloat16 [32, 2048, 2048], P('dp', 'sp'), may hold values from -6 to 6
- proj_pair: bfloat16 [2048, 512], P('dp'), may hold values from -0.03125 to 0.03125
- conv_value: float32 [4, 2048], replicated, may hold values from -3 to 3
- conv_pair: float32 [4, 512], replicated, may hold values from -3 to 3
- step_bias: float32 [32], replicated, may hold values from -1 to 1
- decay_log: float32 [32], replicated, may hold values from -12 to -2
- skip: float32 [32], replicated, may hold values from 0.5 to 1.5
Outputs:
- grad_normed: bfloat16 [32, 2048, 2048], P('dp', 'sp')
- grad_values: bfloat16 [32, 2048, 2048], P('dp', 'sp')
- grad_gate: bfloat16 [32, 2048, 2048], P('dp', 'sp')
- grad_step: bfloat16 [32, 2048, 32], P('dp', 'sp')
- grad_proj: float32 [2048, 512], P('dp')
The draws below stay inside these ranges and needn't reach their ends.
All inputs are finite; a program needn't handle non-finite values.
Results may differ from the reference program's by a relative error of at most 0.02.
Values may be sent and summed in bfloat16 or wider, within the bound.
A program may use at most 128 MiB of HBM per device.

```python
import math
import jax
import jax.numpy as jnp
from jax import lax

D = 2048
HEADS = 32
HEAD = 64
GROUPS = 2
STATE = 128
TAPS = 4
BLOCK = 64
TOK_DEV = 128
INNER = 2048
LENGTH = 2048
BATCH = 32
N_SP = 16


def draw_step_raw(key, part):
    first, second = jax.random.split(jax.random.fold_in(key, 11))
    blocks = LENGTH // TOK_DEV
    shift = jax.random.uniform(first, (BATCH, blocks, 1, HEADS), jnp.float32, -2.0, 1.0)
    noise = jnp.clip(jax.random.normal(second, (BATCH, blocks, TOK_DEV, HEADS), jnp.float32), -3.0, 3.0) * 0.5
    return (shift + noise).reshape(BATCH, LENGTH, HEADS).astype(jnp.bfloat16)


def draw_decay_log(key, part):
    first, second, third = jax.random.split(jax.random.fold_in(key, 23), 3)
    quick_flag = jax.random.randint(first, (HEADS,), 0, 2) == 1
    quick = jnp.exp(jax.random.uniform(second, (HEADS,), jnp.float32, math.log(0.04), math.log(0.12)))
    gentle = jax.random.uniform(third, (HEADS,), jnp.float32, 0.3, 1.0) / LENGTH
    return jnp.log(jnp.where(quick_flag, quick, gentle)).astype(jnp.float32)


def raised(array, own_key, source, target, shards_of, factor):
    def block_of(axis_at):
        return (jnp.arange(array.shape[axis_at]) // (array.shape[axis_at] // shards_of)).reshape((-1,) + (1,) * (array.ndim - 1 - axis_at))

    first = jax.random.permutation(own_key, shards_of)[block_of(target)]
    second = (block_of(target) + shards_of // 2) % shards_of
    return jnp.where((block_of(source) == first) | (block_of(source) == second), factor * array, array)


def block_scale(rng, extent, cuts, least, top_value):
    def one(dim, shards_of):
        heights = jax.random.uniform(jax.random.fold_in(jax.random.fold_in(rng, 6), dim), (shards_of,), jnp.float32, least / len(cuts), top_value / len(cuts))
        return jnp.repeat(jnp.exp(heights), extent[dim] // shards_of).reshape((-1,) + (1,) * (len(extent) - dim - 1))

    level = one(*cuts[0])
    for cut in cuts[1:]:
        level = level * one(*cut)
    return level


def centred(own_key, extent, deviation, bound, pieces=(), kind=jnp.bfloat16):
    loudness = block_scale(own_key, extent, pieces, -0.22, 0.18) if pieces else 1.0
    drawn = jax.random.normal(own_key, extent, jnp.float32) * deviation * loudness
    return jnp.minimum(jnp.maximum(drawn, -bound), bound).astype(kind)


def noise_with(own_key, shape, scale, limit, cuts, heavy, held_as=jnp.bfloat16):
    drawn = scale * jax.random.normal(own_key, shape, jnp.float32)
    if cuts:
        drawn = drawn * block_scale(own_key, shape, cuts, -0.22, 0.18)
    return jnp.clip(raised(drawn, jax.random.fold_in(own_key, 3), *heavy), -limit, limit).astype(held_as)


def setup_inputs(seed: int = 0) -> dict:
    key_list = jax.random.split(jax.random.key(seed), 12)
    normed = noise_with(key_list[0], (BATCH, LENGTH, D), 1.0, 6.0, ((0, 32), (1, 16)), (0, 2, 32, 2.75))
    values = centred(key_list[1], (BATCH, LENGTH, INNER), 1.0, 6.0, ((0, 32), (1, 16)))
    gate_in = centred(key_list[2], (BATCH, LENGTH, INNER), 1.0, 6.0, ((0, 32), (1, 16)))
    step_raw = draw_step_raw(jax.random.fold_in(key_list[11], 71), 0)
    upstream = centred(key_list[4], (BATCH, LENGTH, INNER), 1.0, 6.0, ((0, 32), (1, 16)))
    proj_pair = centred(key_list[5], (D, GROUPS * 2 * STATE), (16 * D) ** -0.5, 0.03125, ((0, 32),))
    conv_value = centred(key_list[6], (TAPS, INNER), TAPS ** -0.5, 3.0, (), jnp.float32)
    conv_pair = centred(key_list[7], (TAPS, GROUPS * 2 * STATE), TAPS ** -0.5, 3.0, (), jnp.float32)
    step_bias = jnp.clip(jax.random.uniform(key_list[8], (HEADS,), jnp.float32, -1.0, 1.0), -1.0, 1.0)
    decay_log = draw_decay_log(jax.random.fold_in(key_list[11], 71), 0)
    skip = jnp.clip(jax.random.uniform(key_list[10], (HEADS,), jnp.float32, 0.5, 1.5), 0.5, 1.5)
    return {"normed": normed, "values": values, "gate_in": gate_in, "step_raw": step_raw, "upstream": upstream, "proj_pair": proj_pair, "conv_value": conv_value, "conv_pair": conv_pair, "step_bias": step_bias, "decay_log": decay_log, "skip": skip}


exact = lax.Precision.HIGHEST

def causal_filter(signal, weights):
    length = signal.shape[0]
    tap_count = weights.shape[0]
    padded = jnp.pad(signal, ((tap_count - 1, 0), (0, 0)))
    summed = jnp.zeros_like(signal)
    for offset in range(tap_count):
        summed = summed + weights[offset] * padded[offset:offset + length]
    return jax.nn.silu(summed)

def silu_slope(gate):
    sig = jax.nn.sigmoid(gate)
    return sig * (1.0 + gate * (1.0 - sig))

def scan_heads(head_value, pair_rows, raw_steps, taps_value, taps_pair, biases, log_rates, skip_gains):
    length, width = head_value.shape
    count = raw_steps.shape[1]
    head_dim = width // count
    state_dim = pair_rows.shape[1] // 2
    blocks = length // BLOCK
    conv_values = causal_filter(head_value, taps_value)
    conv_pairs = causal_filter(pair_rows, taps_pair)
    inject = conv_pairs[:, :state_dim].reshape(blocks, BLOCK, state_dim)
    readout = conv_pairs[:, state_dim:].reshape(blocks, BLOCK, state_dim)
    step_size = jax.nn.softplus(raw_steps + biases[None, :])
    decay_rate = -jnp.exp(log_rates)
    within = jnp.cumsum((step_size * decay_rate[None, :]).reshape(blocks, BLOCK, count), axis=1)
    value_heads = conv_values.reshape(length, count, head_dim)
    scaled = (value_heads * step_size[:, :, None]).reshape(blocks, BLOCK, count, head_dim)
    causal = jnp.tril(jnp.ones((BLOCK, BLOCK), dtype=bool))
    intersect = jnp.einsum('cln,csn->cls', readout, inject, precision=exact)
    spacing = within[:, :, None, :] - within[:, None, :, :]
    weight_diag = jnp.exp(jnp.where(causal[None, :, :, None], spacing, -jnp.inf))
    mixing = intersect[:, :, :, None] * weight_diag
    local_out = jnp.einsum('clsh,cshp->clhp', mixing, scaled, precision=exact)
    to_end = jnp.exp(within[:, -1:, :] - within)
    carried = jnp.einsum('cln,clhp->chpn', inject, scaled * to_end[:, :, :, None], precision=exact)
    block_total = within[:, -1, :]
    running = jnp.cumsum(block_total, axis=0)
    earlier = jnp.tril(jnp.ones((blocks, blocks), dtype=bool), -1)
    link = jnp.exp(jnp.where(earlier[:, :, None], (running - block_total)[:, None, :] - running[None, :, :], -jnp.inf))
    entering = jnp.einsum('cdh,dhpn->chpn', link, carried, precision=exact)
    far_raw = jnp.einsum('cln,chpn->clhp', readout, entering, precision=exact)
    far_out = far_raw * jnp.exp(within)[:, :, :, None]
    direct = (value_heads * skip_gains[None, :, None]).reshape(length, width)
    return (local_out + far_out).reshape(length, width) + direct

def head_grads(head_value, pair_rows, raw_steps, taps_value, taps_pair, biases, log_rates, skip_gains, cotangent):

    def forward(vals, pairs, raws):
        return scan_heads(vals, pairs, raws, taps_value, taps_pair, biases, log_rates, skip_gains)
    output, pullback = jax.vjp(forward, head_value, pair_rows, raw_steps)
    return (output, pullback(cotangent))

def reference(normed, values, gate_in, step_raw, upstream, proj_pair, conv_value, conv_pair, step_bias, decay_log, skip):
    heads_dev = HEADS // N_SP
    width_dev = heads_dev * HEAD
    per_group = N_SP // GROUPS
    pair_width = 2 * STATE
    group_heads = HEADS // GROUPS

    def one_sequence(items):
        token_rows, seq_values, seq_gate, seq_raw, seq_up = items
        pair_pre = jnp.dot(token_rows, proj_pair, preferred_element_type=jnp.float32).astype(jnp.bfloat16)
        gate_float = seq_gate.astype(jnp.float32)
        up_float = seq_up.astype(jnp.float32)
        cot_all = lax.optimization_barrier((up_float * jax.nn.silu(gate_float)).astype(jnp.bfloat16)).astype(jnp.float32)

        def one_device(index):
            first_head = index * heads_dev
            group = first_head // group_heads
            column = first_head * HEAD
            head_value = lax.dynamic_slice_in_dim(seq_values, column, width_dev, 1).astype(jnp.float32)
            pair_rows = lax.dynamic_slice_in_dim(pair_pre, group * pair_width, pair_width, 1).astype(jnp.float32)
            raw_steps = lax.dynamic_slice_in_dim(seq_raw, first_head, heads_dev, 1).astype(jnp.float32)
            taps_value = lax.dynamic_slice_in_dim(conv_value, column, width_dev, 1)
            taps_pair = lax.dynamic_slice_in_dim(conv_pair, group * pair_width, pair_width, 1)
            biases = lax.dynamic_slice_in_dim(step_bias, first_head, heads_dev, 0)
            log_rates = lax.dynamic_slice_in_dim(decay_log, first_head, heads_dev, 0)
            skip_gains = lax.dynamic_slice_in_dim(skip, first_head, heads_dev, 0)
            cotangent = lax.dynamic_slice_in_dim(cot_all, column, width_dev, 1)
            output, grads = head_grads(head_value, pair_rows, raw_steps, taps_value, taps_pair, biases, log_rates, skip_gains, cotangent)
            return (output.astype(jnp.bfloat16), grads[0].astype(jnp.bfloat16), grads[1].astype(jnp.bfloat16), grads[2].astype(jnp.bfloat16))
        outputs, value_grads, pair_grads, step_grads = lax.map(one_device, jnp.arange(N_SP, dtype=jnp.int32))
        side = jnp.moveaxis(outputs, 0, 1).reshape(LENGTH, INNER)
        grad_gate = (up_float * lax.optimization_barrier(side).astype(jnp.float32) * silu_slope(gate_float)).astype(jnp.bfloat16)
        grad_values = jnp.moveaxis(value_grads, 0, 1).reshape(LENGTH, INNER)
        grad_step = jnp.moveaxis(step_grads, 0, 1).reshape(LENGTH, HEADS)
        device_part = lax.optimization_barrier(pair_grads)
        group_sum = device_part.astype(jnp.float32).reshape(GROUPS, per_group, LENGTH, pair_width).sum(axis=1)
        pair_total = jnp.moveaxis(group_sum, 0, 1).reshape(LENGTH, GROUPS * pair_width).astype(jnp.bfloat16)
        grad_normed = lax.dot_general(pair_total, proj_pair, (((1,), (1,)), ((), ())), preferred_element_type=jnp.float32).astype(jnp.bfloat16)
        grad_proj = lax.dot_general(token_rows, pair_total, (((0,), (0,)), ((), ())), preferred_element_type=jnp.float32)
        return (grad_normed, grad_values, grad_gate, grad_step, grad_proj)
    results = lax.map(one_sequence, (normed, values, gate_in, step_raw, upstream))
    return (results[0], results[1], results[2], results[3], lax.optimization_barrier(jnp.sum(results[4], axis=0)))
```

```python
import functools

import jax
import jax.numpy as jnp
from jax import lax
from jax.experimental import pallas as pl
from jax.experimental.pallas import tpu as pltpu
from jax.sharding import PartitionSpec as P

HEADS = 32
HEAD = 64
GROUPS = 2
STATE = 128
TOK = 128
PAIRS = 16
TAPS = 4
CHUNKS = 16
RATIO = 3
MESH = pl.DeviceIdType.MESH
f32 = jnp.float32
bf16 = jnp.bfloat16
VM = pl.BlockSpec(memory_space=pltpu.VMEM)
SM = pl.BlockSpec(memory_space=pltpu.SMEM)
ANY = pl.BlockSpec(memory_space=pl.ANY)


def dot(a, b, ca, cb, precision=None):
    return lax.dot_general(
        a, b, (((ca,), (cb,)), ((), ())), precision=precision, preferred_element_type=f32
    )


def sigmoid(v):
    return 1.0 / (1.0 + jnp.exp(-v))


def remote(src, dst, send, recv, where):
    return pltpu.make_async_remote_copy(
        src_ref=src, dst_ref=dst, send_sem=send, recv_sem=recv, device_id=where, device_id_type=MESH
    )


def meet(places):
    barrier = pltpu.get_barrier_semaphore()
    for where in places:
        pl.semaphore_signal(barrier, inc=1, device_id=where, device_id_type=MESH)
    pl.semaphore_wait(barrier, len(places))


def gather_kernel(chips, n_sp, proj, values, normed, full, halo, ss, rs, fs, fr, hs, hr):
    z, d = lax.axis_index("sp"), lax.axis_index("dp")
    m, c = d // 2, lax.rem(d, 2)
    partner = {"dp": 2 * m + 1 - c}
    after, before = {"sp": lax.rem(z + 1, n_sp)}, {"sp": lax.rem(z + n_sp - 1, n_sp)}
    others = [lax.rem(m + k, chips) for k in range(1, chips)]
    meet([{"dp": 2 * t + c} for t in others] + [partner, after, before])
    sends = []
    for i, ref in enumerate((values, normed)):
        sends.append(remote(ref.at[0, pl.ds(TOK - 16, 16), :], halo.at[i], hs.at[i], hr.at[i], after))
    sends.append(remote(proj, full.at[m, c], fs.at[m], fr.at[m], partner))
    for k, t in enumerate(others):
        sends.append(remote(proj, full.at[m, c], ss.at[k], rs.at[m], {"dp": 2 * t + c}))
    for copy in sends:
        copy.start()
    full[m, c] = proj[...]
    for k in range(1, chips):
        src = lax.rem(m + chips - k, chips)
        remote(proj, full.at[src, c], ss.at[0], rs.at[src], partner).wait_recv()
        copy = remote(full.at[src, c], full.at[src, c], fs.at[src], fr.at[src], partner)
        copy.start()
        sends.append(copy)
    for src in range(chips):
        remote(proj, full.at[src, 1 - c], ss.at[0], fr.at[src], partner).wait_recv()
    for i in range(2):
        remote(halo.at[i], halo.at[i], hs.at[i], hr.at[i], after).wait_recv()
    for copy in sends:
        copy.wait_send()


def gather(proj, values, normed, chips, n_sp):
    rows, cols = proj.shape
    dma = pltpu.SemaphoreType.DMA
    return pl.pallas_call(
        functools.partial(gather_kernel, chips, n_sp),
        out_shape=(
            jax.ShapeDtypeStruct((chips, 2, rows, cols), bf16),
            jax.ShapeDtypeStruct((2, 16, values.shape[2]), bf16),
        ),
        in_specs=[VM, ANY, ANY],
        out_specs=(VM, VM),
        scratch_shapes=[dma((chips,)), dma((chips,)), dma((chips,)), dma((chips,)), dma((2,)), dma((2,))],
        compiler_params=pltpu.CompilerParams(collective_id=0, has_side_effects=True),
        name="gather",
    )(proj, values, normed)


def steps(raw_ref, bias_ref, log_ref):
    v = raw_ref[0].astype(f32) + bias_ref[...]
    dt = jnp.maximum(v, 0.0) + jnp.log1p(jnp.exp(-jnp.abs(v)))
    rate = -jnp.exp(log_ref[...])
    a = dt * rate
    row = lax.broadcasted_iota(jnp.int32, (TOK, TOK), 0)
    col = lax.broadcasted_iota(jnp.int32, (TOK, TOK), 1)
    lower = (col <= row).astype(f32)
    acum = dot(lower, a, 1, 0, lax.Precision.HIGHEST)
    acum_t = dot(a, lower, 0, 1, lax.Precision.HIGHEST)
    return v, dt, rate, acum, acum_t


def column(mat, h):
    lane = lax.broadcasted_iota(jnp.int32, mat.shape, 1)
    return jnp.sum(jnp.where(lane == h, mat, 0.0), axis=1, keepdims=True)


def first_half(rows=TOK):
    return lax.broadcasted_iota(jnp.int32, (rows, 128), 1) < HEAD


def pair_columns(mat, j):
    return jnp.where(first_half(mat.shape[0]), column(mat, 2 * j), column(mat, 2 * j + 1))


def slab(j):
    return pl.ds(pl.multiple_of(j * 128, 128), 128)


def conv_slab(ext, taps, cs):
    total = taps[0:1, cs] * ext[13 : 13 + TOK, cs]
    for k in range(1, TAPS):
        total = total + taps[k : k + 1, cs] * ext[13 + k : 13 + k + TOK, cs]
    return total


def extended(ext, halo, main, z):
    ext[0:16, :] = jnp.where(z > 0, halo.astype(f32), 0.0)
    ext[16 : 16 + TOK, :] = main.astype(f32)


def local_kernel(
    z_ref, full, normed, values, gate, up, raw, halo, taps_v, taps_p, bias, logs,
    bc_out, slope_out, left_out, right_out, dec_out, yl_out, dxl_out, dg_out,
    vext, pext, at_ref,
):
    z = z_ref[0]
    proj = full[...]
    pext[16 : 16 + TOK, :] = dot(normed[0], proj, 1, 0).astype(bf16).astype(f32)
    before = dot(halo[1], proj, 1, 0).astype(bf16).astype(f32)
    pext[0:16, :] = jnp.where(z > 0, before, 0.0)
    extended(vext, halo[0], values[0], z)
    _, dt, _, acum, acum_t = steps(raw, bias, logs)
    at_ref[...] = acum_t
    dec_out[...] = jnp.exp(jnp.broadcast_to(acum_t[:, TOK - 1 : TOK], (HEADS, 128)))
    for q in range(4):
        cs = slice(q * 128, q * 128 + 128)
        p = conv_slab(pext, taps_p, cs)
        sig = sigmoid(p)
        bc_out[:, cs] = p * sig
        slope_out[:, cs] = sig * (1.0 + p * (1.0 - sig))
    row = lax.broadcasted_iota(jnp.int32, (TOK, TOK), 0)
    col = lax.broadcasted_iota(jnp.int32, (TOK, TOK), 1)
    causal = col <= row
    half = first_half()
    for g in range(GROUPS):
        inject = bc_out[:, 256 * g : 256 * g + 128].astype(bf16)
        readout = bc_out[:, 256 * g + 128 : 256 * g + 256].astype(bf16)
        cross = dot(readout, inject, 1, 1)
        dg_out[g] = jnp.zeros((TOK, TOK), f32)

        def body(i, carry, g=g, inject=inject, readout=readout, cross=cross):
            j = g * (PAIRS // GROUPS) + i
            cs = slab(j)
            x = conv_slab(vext, taps_v, cs)
            u = x * sigmoid(x)
            a0, a1 = column(acum, 2 * j), column(acum, 2 * j + 1)
            ac = jnp.where(half, a0, a1)
            end = ac[TOK - 1 : TOK, :]
            xd = u * pair_columns(dt, j)
            v = gate[0, :, cs].astype(f32)
            cot = (up[0, :, cs].astype(f32) * v * sigmoid(v)).astype(bf16)
            xde = (xd * jnp.exp(end - ac)).astype(bf16)
            dye = (cot.astype(f32) * jnp.exp(ac)).astype(bf16)
            left_out[cs, :] = dot(xde, inject, 0, 0)
            right_out[cs, :] = dot(dye, readout, 0, 0)
            zero = jnp.zeros((), bf16)
            xb = xd.astype(bf16)
            xd0, xd1 = jnp.where(half, xb, zero), jnp.where(half, zero, xb)
            dy0, dy1 = jnp.where(half, cot, zero), jnp.where(half, zero, cot)
            l0 = jnp.exp(jnp.where(causal, a0 - at_ref[pl.ds(2 * j, 1), :], -jnp.inf))
            l1 = jnp.exp(jnp.where(causal, a1 - at_ref[pl.ds(2 * j + 1, 1), :], -jnp.inf))
            w0, w1 = (cross * l0).astype(bf16), (cross * l1).astype(bf16)
            yl_out[:, cs] = dot(w0, xd0, 1, 0) + dot(w1, xd1, 1, 0)
            dxl_out[:, cs] = dot(w0, dy0, 0, 0) + dot(w1, dy1, 0, 0)
            dg_out[g] += dot(dy0, xb, 1, 1) * l0 + dot(dy1, xb, 1, 1) * l1
            return carry

        lax.fori_loop(0, PAIRS // GROUPS, body, 0)


def local(z, full, normed, values, gate, up, raw, halo, taps_v, taps_p, bias, logs):
    width = values.shape[2]
    s = jax.ShapeDtypeStruct
    return pl.pallas_call(
        local_kernel,
        out_shape=(
            s((TOK, 512), f32), s((TOK, 512), f32), s((width, STATE), f32), s((width, STATE), f32),
            s((HEADS, 128), f32), s((TOK, width), f32), s((TOK, width), f32), s((GROUPS, TOK, TOK), f32),
        ),
        in_specs=[SM] + [VM] * 11,
        out_specs=(VM,) * 8,
        scratch_shapes=[
            pltpu.VMEM((16 + TOK, width), f32), pltpu.VMEM((16 + TOK, 512), f32), pltpu.VMEM((HEADS, TOK), f32),
        ],
        name="local",
    )(z, full, normed, values, gate, up, raw, halo, taps_v, taps_p, bias, logs)


def chain_kernel(n_sp, left, right, dec, s_in, ds_out, f_out, b_out, fs, fr, bs, br):
    z = lax.axis_index("sp")
    after, before = {"sp": lax.rem(z + 1, n_sp)}, {"sp": lax.rem(z + n_sp - 1, n_sp)}
    meet([after, before])
    rows = HEADS * HEAD // CHUNKS
    heads = HEADS // CHUNKS

    @pl.when(z == 0)
    def _():
        s_in[...] = jnp.zeros_like(s_in)

    @pl.when(z == n_sp - 1)
    def _():
        ds_out[...] = jnp.zeros_like(ds_out)

    def part(k):
        return pl.ds(pl.multiple_of(k * rows, rows), rows)

    def step(k, got, mine, out, send, recv, has, gives, where):
        at = part(k)
        copy = remote(out.at[at, :], got.at[at, :], send.at[k], recv.at[k], where)

        @pl.when(has)
        def _():
            copy.wait_recv()

        for i in range(heads):
            hs = pl.ds(pl.multiple_of(k * rows + i * HEAD, HEAD), HEAD)
            new = dec[pl.ds(k * heads + i, 1), :] * got[hs, :].astype(f32) + mine[hs, :]
            out[hs, :] = new.astype(bf16)

        @pl.when(gives)
        def _():
            copy.start()

    def tick(t, carry):
        kf = t - z * RATIO
        kb = t - (n_sp - 1 - z) * RATIO

        @pl.when((kf >= 0) & (kf < CHUNKS))
        def _():
            step(kf, s_in, left, f_out, fs, fr, z > 0, z < n_sp - 1, after)

        @pl.when((kb >= 0) & (kb < CHUNKS))
        def _():
            step(kb, ds_out, right, b_out, bs, br, z < n_sp - 1, z > 0, before)

        return carry

    lax.fori_loop(0, (n_sp - 1) * RATIO + CHUNKS, tick, 0)

    def finish(k, carry):
        at = part(k)

        @pl.when(z < n_sp - 1)
        def _():
            remote(f_out.at[at, :], s_in.at[at, :], fs.at[k], fr.at[k], after).wait_send()

        @pl.when(z > 0)
        def _():
            remote(b_out.at[at, :], ds_out.at[at, :], bs.at[k], br.at[k], before).wait_send()

        return carry

    lax.fori_loop(0, CHUNKS, finish, 0)


def chain(left, right, dec, n_sp):
    shape = jax.ShapeDtypeStruct(left.shape, bf16)
    dma = pltpu.SemaphoreType.DMA
    return pl.pallas_call(
        functools.partial(chain_kernel, n_sp),
        out_shape=(shape, shape),
        in_specs=[VM] * 3,
        out_specs=(VM, VM),
        scratch_shapes=[pltpu.VMEM(left.shape, bf16), pltpu.VMEM(left.shape, bf16)] + [dma((CHUNKS,))] * 4,
        compiler_params=pltpu.CompilerParams(collective_id=1, has_side_effects=True),
        name="chain",
    )(left, right, dec)


def grads_kernel(
    z_ref, values, gate, up, raw, halo, taps_v, taps_p, bias, logs, skips,
    bc, slope, left, dec, s_in, ds_out, yl, dxl, dg,
    gv_out, gg_out, gs_out, gv_tail, gv_halo, dp_out, dp_halo, dp_tail, dp_before,
    vext, dxs, dps, dbc, da_ref, dd_ref,
):
    z = z_ref[0]
    extended(vext, halo[0], values[0], z)
    v_step, dt, rate, acum, _ = steps(raw, bias, logs)
    half = first_half()
    keep = z > 0
    da_ref[...] = jnp.zeros_like(da_ref)
    dd_ref[...] = jnp.zeros_like(dd_ref)
    dxs[0:16, :] = jnp.zeros((16, 128), f32)
    dxs[16 + TOK :, :] = jnp.zeros((8, 128), f32)
    dps[0:16, :] = jnp.zeros((16, 512), f32)
    dps[16 + TOK :, :] = jnp.zeros((8, 512), f32)
    head_lane = lax.broadcasted_iota(jnp.int32, (TOK, HEADS), 1)
    last = lax.broadcasted_iota(jnp.int32, (TOK, HEADS), 0) == TOK - 1
    for g in range(GROUPS):
        inject = bc[:, 256 * g : 256 * g + 128].astype(bf16)
        readout = bc[:, 256 * g + 128 : 256 * g + 256].astype(bf16)
        dgb = dg[g].astype(bf16)
        dbc[:, 256 * g : 256 * g + 128] = dot(dgb, readout, 0, 0)
        dbc[:, 256 * g + 128 : 256 * g + 256] = dot(dgb, inject, 1, 0)

        def body(i, carry, g=g, inject=inject, readout=readout):
            j = g * (PAIRS // GROUPS) + i
            cs = slab(j)
            x = conv_slab(vext, taps_v, cs)
            sig = sigmoid(x)
            u = x * sig
            ac = pair_columns(acum, j)
            ea, ee = jnp.exp(ac), jnp.exp(ac[TOK - 1 : TOK, :] - ac)
            dtc = pair_columns(dt, j)
            xd = u * dtc
            v = gate[0, :, cs].astype(f32)
            upv = up[0, :, cs].astype(f32)
            gsig = sigmoid(v)
            cot = (upv * v * gsig).astype(bf16).astype(f32)
            xde, dye = (xd * ee).astype(bf16), (cot * ea).astype(bf16)
            s, ds = s_in[cs, :], ds_out[cs, :]
            y = yl[:, cs] + ea * dot(readout, s, 1, 1)
            dxd = dxl[:, cs] + ee * dot(inject, ds, 1, 1)
            dbc[:, 256 * g + 128 : 256 * g + 256] += dot(dye, s, 1, 0)
            dbc[:, 256 * g : 256 * g + 128] += dot(xde, ds, 1, 0)
            d0, d1 = dec[pl.ds(2 * j, 1), :], dec[pl.ds(2 * j + 1, 1), :]
            lf, sf, df = left[cs, :], s.astype(f32), ds.astype(f32)
            e0 = jnp.sum((d0 * sf[:HEAD] + lf[:HEAD]) * df[:HEAD])
            e1 = jnp.sum((d1 * sf[HEAD:] + lf[HEAD:]) * df[HEAD:])
            pa = cot * y - xd * dxd
            pd = u * dxd
            is0, is1 = head_lane == 2 * j, head_lane == 2 * j + 1
            sum0 = jnp.sum(jnp.where(half, pa, 0.0), axis=1, keepdims=True)
            sum1 = jnp.sum(jnp.where(half, 0.0, pa), axis=1, keepdims=True)
            da_ref[...] += jnp.where(is0, sum0 + jnp.where(last, e0, 0.0), 0.0) + jnp.where(
                is1, sum1 + jnp.where(last, e1, 0.0), 0.0
            )
            sum0 = jnp.sum(jnp.where(half, pd, 0.0), axis=1, keepdims=True)
            sum1 = jnp.sum(jnp.where(half, 0.0, pd), axis=1, keepdims=True)
            dd_ref[...] += jnp.where(is0, sum0, 0.0) + jnp.where(is1, sum1, 0.0)
            sk = skips[0:1, cs]
            ybf = (y + sk * u).astype(bf16).astype(f32)
            gg_out[0, :, cs] = (upv * ybf * (gsig * (1.0 + v * (1.0 - gsig)))).astype(bf16)
            du = dtc * dxd + sk * cot
            dxs[16 : 16 + TOK, :] = du * (sig * (1.0 + x * (1.0 - sig)))
            dv = taps_v[0:1, cs] * dxs[3 : 3 + 16 + TOK, :]
            for k in range(1, TAPS):
                dv = dv + taps_v[k : k + 1, cs] * dxs[3 - k : 3 - k + 16 + TOK, :]
            gv_out[0, :, cs] = dv[16:].astype(bf16)
            gv_tail[:, cs] = dv[TOK:]
            gv_halo[:, cs] = jnp.where(keep, dv[0:16], 0.0)
            return carry

        lax.fori_loop(0, PAIRS // GROUPS, body, 0)
    row = lax.broadcasted_iota(jnp.int32, (TOK, TOK), 0)
    col = lax.broadcasted_iota(jnp.int32, (TOK, TOK), 1)
    da = dot((col >= row).astype(f32), da_ref[...], 1, 0, lax.Precision.HIGHEST)
    gs_out[0] = ((rate * da + dd_ref[...]) * sigmoid(v_step)).astype(bf16)
    for q in range(4):
        cs = slice(q * 128, q * 128 + 128)
        dps[16 : 16 + TOK, cs] = dbc[:, cs] * slope[:, cs]
        dp = taps_p[0:1, cs] * dps[3 : 3 + 16 + TOK, cs]
        for k in range(1, TAPS):
            dp = dp + taps_p[k : k + 1, cs] * dps[3 - k : 3 - k + 16 + TOK, cs]
        dp_out[:, cs] = dp[16:].astype(bf16)
        dp_tail[:, cs] = dp[TOK:]
        before = jnp.where(keep, dp[0:16], 0.0)
        dp_before[:, cs] = before
        dp_halo[:, cs] = before.astype(bf16)


def grads(z, values, gate, up, raw, halo, taps_v, taps_p, bias, logs, skips, *rest):
    width = values.shape[2]
    s = jax.ShapeDtypeStruct
    return pl.pallas_call(
        grads_kernel,
        out_shape=(
            s((1, TOK, width), bf16), s((1, TOK, width), bf16), s((1, TOK, HEADS), bf16),
            s((16, width), f32), s((16, width), f32),
            s((TOK, 512), bf16), s((16, 512), bf16), s((16, 512), f32), s((16, 512), f32),
        ),
        in_specs=[SM] + [VM] * 19,
        out_specs=(VM,) * 9,
        scratch_shapes=[
            pltpu.VMEM((16 + TOK, width), f32), pltpu.VMEM((24 + TOK, 128), f32),
            pltpu.VMEM((24 + TOK, 512), f32), pltpu.VMEM((TOK, 512), f32),
            pltpu.VMEM((TOK, HEADS), f32), pltpu.VMEM((TOK, HEADS), f32),
        ],
        name="grads",
    )(z, values, gate, up, raw, halo, taps_v, taps_p, bias, logs, skips, *rest)


def reduce_kernel(
    chips, n_sp, normed, halo, dp, dp_halo, gv_halo, dp_before,
    out, gv_after, dp_after,
    mine, theirs, both, planes, zs, zr, zb, zc,
    cs_, cr, ps, pr, as_, ar, bs, br, hs, hr,
):
    z, d = lax.axis_index("sp"), lax.axis_index("dp")
    m, c = d // 2, lax.rem(d, 2)
    partner = {"dp": 2 * m + 1 - c}
    before = {"sp": lax.rem(z + n_sp - 1, n_sp)}
    plane = [lax.rem(m + k, chips) for k in range(1, chips)]
    line = [lax.rem(z + k, n_sp) for k in range(1, n_sp)]
    meet([{"dp": 2 * t + c} for t in plane] + [partner] + [{"sp": t} for t in line])
    sends = [
        remote(gv_halo, gv_after, hs.at[0], hr.at[0], before),
        remote(dp_before, dp_after, hs.at[1], hr.at[1], before),
    ]
    for copy in sends:
        copy.start()
    order = plane + [m]
    for k, t in enumerate(order):
        at = slab(t)
        block = dot(normed[0, :, at], dp[...], 0, 0) + dot(halo[1, :, at], dp_halo[...], 0, 0)
        mine[t] = block.astype(bf16).reshape(mine.shape[1:])
        copy = remote(mine.at[t, 1 - c], theirs.at[t], cs_.at[k], cr.at[t], partner)
        copy.start()
        sends.append(copy)
    for k, t in enumerate(order):
        remote(mine.at[t, 0], theirs.at[t], cs_.at[k], cr.at[t], partner).wait_recv()
        both[t] = (mine[t, c].astype(f32) + theirs[t].astype(f32)).astype(bf16)
        if k < chips - 1:
            copy = remote(both.at[t], planes.at[m], ps.at[k], pr.at[m], {"dp": 2 * t + c})
            copy.start()
            sends.append(copy)
    total = both[m].astype(f32)
    for k in range(1, chips):
        t = lax.rem(m + chips - k, chips)
        remote(both.at[t], planes.at[t], ps.at[0], pr.at[t], partner).wait_recv()
        total = total + planes[t].astype(f32)
    per = 16 // n_sp
    for q in range(16):
        tile = total[16 * (q // 4) : 16 * (q // 4) + 16, 128 * (q % 4) : 128 * (q % 4) + 128]
        zs[q // per, 16 * (q % per) : 16 * (q % per) + 16, :] = tile.astype(bf16)
    for k, t in enumerate(line):
        copy = remote(zs.at[t], zr.at[z], as_.at[k], ar.at[z], {"sp": t})
        copy.start()
        sends.append(copy)
    total = zs[z].astype(f32)
    for k in range(1, n_sp):
        t = lax.rem(z + n_sp - k, n_sp)
        remote(zs.at[t], zr.at[t], as_.at[0], ar.at[t], before).wait_recv()
        total = total + zr[t].astype(f32)
    zb[...] = total.astype(bf16)
    for k, t in enumerate(line):
        copy = remote(zb, zc.at[z], bs.at[k], br.at[z], {"sp": t})
        copy.start()
        sends.append(copy)
    zc[z] = zb[...]
    for k in range(1, n_sp):
        t = lax.rem(z + n_sp - k, n_sp)
        remote(zb, zc.at[t], bs.at[0], br.at[t], before).wait_recv()
    for q in range(16):
        tile = zc[q // per, 16 * (q % per) : 16 * (q % per) + 16, :].astype(f32)
        out[16 * (q // 4) : 16 * (q // 4) + 16, 128 * (q % 4) : 128 * (q % 4) + 128] = tile
    sends[0].wait_recv()
    sends[1].wait_recv()
    for copy in sends:
        copy.wait_send()


def reduce(normed, halo, dp, dp_halo, gv_halo, dp_before, chips, n_sp):
    dma = pltpu.SemaphoreType.DMA
    s = jax.ShapeDtypeStruct
    per = 16 // n_sp * 16
    return pl.pallas_call(
        functools.partial(reduce_kernel, chips, n_sp),
        out_shape=(s((64, 512), f32), s(gv_halo.shape, f32), s(dp_before.shape, f32)),
        in_specs=[VM] * 6,
        out_specs=(VM,) * 3,
        scratch_shapes=[
            pltpu.VMEM((chips, 2, 64, 512), bf16), pltpu.VMEM((chips, 64, 512), bf16),
            pltpu.VMEM((chips, 64, 512), bf16), pltpu.VMEM((chips, 64, 512), bf16),
            pltpu.VMEM((n_sp, per, 128), bf16), pltpu.VMEM((n_sp, per, 128), bf16),
            pltpu.VMEM((per, 128), bf16), pltpu.VMEM((n_sp, per, 128), bf16),
            dma((chips,)), dma((chips,)), dma((chips,)), dma((chips,)),
            dma((n_sp,)), dma((n_sp,)), dma((n_sp,)), dma((n_sp,)), dma((2,)), dma((2,)),
        ],
        compiler_params=pltpu.CompilerParams(collective_id=2, has_side_effects=True),
        name="reduce",
    )(normed, halo, dp, dp_halo, gv_halo, dp_before)


def finish_kernel(full, dp, dp_tail, dp_after, gv_tail, gv_after, gv_in, gn_out, gv_out):
    end = (dp_tail[...] + dp_after[...]).astype(bf16)
    dpair = jnp.concatenate([dp[0 : TOK - 16, :], end], axis=0)
    for q in range(full.shape[0] // 256):
        gn_out[0, :, 256 * q : 256 * q + 256] = dot(dpair, full[256 * q : 256 * q + 256, :], 1, 1).astype(bf16)
    gv_out[0] = (gv_tail[...] + gv_after[...]).astype(bf16)


def finish(full, dp, dp_tail, dp_after, gv_tail, gv_after, gv):
    s = jax.ShapeDtypeStruct
    whole = lambda a: pl.BlockSpec(a.shape, lambda i: (0,) * a.ndim)
    return pl.pallas_call(
        finish_kernel,
        grid=(1,),
        out_shape=(s((1, TOK, full.shape[0]), bf16), s(gv.shape, bf16)),
        in_specs=[whole(a) for a in (full, dp, dp_tail, dp_after, gv_tail, gv_after)] + [ANY],
        out_specs=(
            pl.BlockSpec((1, TOK, full.shape[0]), lambda i: (0, 0, 0)),
            pl.BlockSpec((1, 16, gv.shape[2]), lambda i: (0, TOK // 16 - 1, 0)),
        ),
        input_output_aliases={6: 1},
        name="finish",
    )(full, dp, dp_tail, dp_after, gv_tail, gv_after, gv)


def per_device(
    n_sp, n_dp, normed, values, gate_in, step_raw, upstream, proj_pair,
    conv_value, conv_pair, step_bias, decay_log, skip,
):
    z = lax.axis_index("sp").astype(jnp.int32).reshape(1)
    bias, logs = step_bias.reshape(1, HEADS), decay_log.reshape(1, HEADS)
    skips = jnp.repeat(skip, HEAD).reshape(1, HEADS * HEAD)
    chips = n_dp // 2
    full, halo = gather(proj_pair, values, normed, chips, n_sp)
    full = full.reshape(-1, full.shape[-1])
    bc, slope, left, right, dec, yl, dxl, dg = local(
        z, full, normed, values, gate_in, upstream, step_raw, halo, conv_value, conv_pair, bias, logs
    )
    s_in, ds_out = chain(left, right, dec, n_sp)
    gv, gg, gs, gv_tail, gv_halo, dp, dp_halo, dp_tail, dp_before = grads(
        z, values, gate_in, upstream, step_raw, halo, conv_value, conv_pair, bias, logs, skips,
        bc, slope, left, dec, s_in, ds_out, yl, dxl, dg,
    )
    gp, gv_after, dp_after = reduce(normed, halo, dp, dp_halo, gv_halo, dp_before, chips, n_sp)
    gn, gv = finish(full, dp, dp_tail, dp_after, gv_tail, gv_after, gv)
    return gn, gv, gg, gs, gp


def solution(mesh):
    tokens = P("dp", "sp", None)
    return jax.shard_map(
        functools.partial(per_device, mesh.shape["sp"], mesh.shape["dp"]),
        mesh=mesh,
        in_specs=(tokens,) * 5 + (P("dp", None),) + (P(),) * 5,
        out_specs=(tokens,) * 4 + (P("dp", None),),
        check_vma=False,
    )
```
